128 devices in a mesh: ep: 32 (over z, y, core), tp: 4 (over x).
Axes of the slice: x: 4, y: 4, z: 4, core: 2. Of those that a mesh axis runs over, the one named last changes fastest.
Arguments:
- tokens: bfloat16 [16384, 2048], P(('ep', 'tp')), may hold values from -6 to 6
- norm_gain: float32 [2048], replicated, may hold values from 0.1 to 1.9
- expert_ids: int32 [16384, 2], P('ep'), may hold values from 0 to 31, all different within a row; in each aligned block of 128 rows (0 to 127, 128 to 255, ...) at most 10 rows name the same one
- route_weight: float32 [16384, 2], P('ep'), may hold values from 0.1 to 1
- exp_gate: bfloat16 [32, 2048, 7168], P('ep', None, 'tp'), may hold values from -0.125 to 0.125
- exp_up: bfloat16 [32, 2048, 7168], P('ep', None, 'tp'), may hold values from -0.125 to 0.125
- exp_down: bfloat16 [32, 7168, 2048], P('ep', 'tp'), may hold values from -0.0625 to 0.0625
Outputs:
- mixed: bfloat16 [16384, 2048], P(('ep', 'tp'))
The draws below stay inside these ranges and needn't reach their ends.
Inputs may be any that keep to these rules, and one draw needn't show every extreme that they name: `expert_ids`: A row names 2 different experts. Within each aligned block of 128 rows (the tokens of one device) no expert is named by more than 10 rows, and in some block one expert is named by exactly 10 rows.
All inputs are finite; a program needn't handle non-finite values.
Results may differ from the reference program's by a relative error of at most 0.012.
Values may be sent and summed in bfloat16 or wider, within the bound.
A program may use at most 128 MiB of HBM per device.

```python
import math
import jax
import jax.numpy as jnp
import numpy as np
from jax import lax

D = 2048
FF = 7168
TOPK = 2
TOK_DEV = 128
EXPERTS = 32
CAP = 10
TOKENS = 16384
N_EP = 32
N_TP = 4


def level_of(stream_key, extent, cuts, smallest, largest):
    level, own = 1.0, jax.random.fold_in(stream_key, 6)
    for axis_at, shards_of in cuts:
        draws = jnp.exp(jax.random.uniform(jax.random.fold_in(own, axis_at), (shards_of,), jnp.float32, smallest / len(cuts), largest / len(cuts)))
        level = level * jnp.repeat(draws, extent[axis_at] // shards_of).reshape([-1 if axis == axis_at else 1 for axis in range(len(extent))])
    return level


def shared_out(key, own, number, rows, number_of, top, limit, slope):
    order = jax.random.permutation(key, number_of)
    crowded, ordinary = portions_of(number_of, rows * top, limit, slope, True), portions_of(number_of, rows * top, limit, slope, False)
    places = jnp.arange(number_of)

    def named(tallies, turn):
        used = int((tallies > 0).sum())
        fixed = max(1, used // 4)
        passed = fixed + (places - fixed + turn * (used - fixed)) % max(1, number_of - fixed)
        return jnp.zeros((number_of,), jnp.int32).at[order[jnp.where(places < fixed, places, passed)]].set(jnp.asarray(tallies, jnp.int32))

    tallies = jnp.where(number % 4 == 0, named(crowded, number // 4), named(ordinary, number - number // 4 - 1))
    mixed = jax.random.permutation(jax.random.fold_in(own, 3), number_of)
    donor, sink = mixed[0:number_of // 2 * 2:2], mixed[1:number_of // 2 * 2:2]
    margin = jnp.minimum(tallies[donor] - 1, limit - tallies[sink]) // 2
    margin = jnp.where((donor == order[0]) | (sink == order[0]) | (tallies[sink] == 0), 0, jnp.maximum(margin, 0))
    passed = jax.random.randint(jax.random.fold_in(own, 4), (number_of // 2,), 0, 1 << 20) % (margin + 1)
    tallies = tallies.at[donor].add(-passed).at[sink].add(passed)
    labels = jnp.searchsorted(jnp.cumsum(tallies), jnp.arange(rows * top), side="right").astype(jnp.int32)
    table = labels.reshape(top, rows).T
    table = table[jax.random.permutation(jax.random.fold_in(own, 1), rows)]
    turn = jax.random.randint(jax.random.fold_in(own, 2), (rows, 1), 0, top)
    return jnp.take_along_axis(table, (jnp.arange(top)[None, :] + turn) % top, axis=1)


def portions_of(amount, total, most, skew, full):
    loads = [(1 << 20) // math.isqrt(standing ** skew) + 1 for standing in range(1, amount + 1)]
    largest = most if full else min(most, max(-(-total // amount), total * loads[0] // sum(loads)))
    least = 1 if total - largest >= amount - 1 else 0
    holding, spare = [largest] + [least] * (amount - 1), total - largest - least * (amount - 1)
    while spare > 0:
        candidates = [i for i in range(1, amount) if holding[i] < largest] or [i for i in range(1, amount) if holding[i] < most]
        mass, remaining = sum([loads[i] for i in candidates]), spare
        for i in candidates:
            more = min(most - holding[i], max(1, remaining * loads[i] // mass), spare)
            holding[i] = holding[i] + more
            spare = spare - more
    return np.array(holding)


def gaussian(own_key, shape, spread, limit, cuts=(), kind=jnp.bfloat16):
    array = jax.random.normal(own_key, shape, jnp.float32) * spread
    if len(cuts) > 0:
        array = level_of(own_key, shape, cuts, -0.22, 0.18) * array
    return jnp.clip(array, min=-limit, max=limit).astype(kind)


def setup_inputs(seed: int = 0) -> dict:
    keys = jax.random.split(jax.random.key(seed), 8)
    tokens = gaussian(keys[0], (TOKENS, D), 1.0, 6.0, ((0, 128),))
    norm_gain = jnp.clip(1.0 + 0.18 * jax.random.normal(keys[1], (D,), jnp.float32), 0.1, 1.9)
    expert_ids_keys = jax.random.split(jax.random.fold_in(keys[2], 1), TOKENS // TOK_DEV)
    expert_ids_turns = jax.random.permutation(jax.random.fold_in(keys[2], 3), TOKENS // TOK_DEV)
    expert_ids = jax.vmap(lambda own, number: shared_out(jax.random.fold_in(keys[2], 2), own, number, TOK_DEV, EXPERTS, TOPK, CAP, 2))(expert_ids_keys, expert_ids_turns).reshape((TOKENS, TOPK))
    route_weight = jnp.clip(0.1 + 0.9 * jax.random.uniform(keys[3], (TOKENS, TOPK), jnp.float32) ** level_of(keys[3], (TOKENS, TOPK), ((0, 32),), -0.2, 0.2), 0.1, 1.0)
    exp_gate = gaussian(keys[4], (EXPERTS, D, FF), D ** -0.5, 0.125, ((0, 32), (2, 4)))
    exp_up = gaussian(keys[5], (EXPERTS, D, FF), D ** -0.5, 0.125, ((0, 32), (2, 4)))
    exp_down = gaussian(keys[6], (EXPERTS, FF, D), FF ** -0.5, 0.0625, ((0, 32), (1, 4)))
    return {"tokens": tokens, "norm_gain": norm_gain, "expert_ids": expert_ids, "route_weight": route_weight, "exp_gate": exp_gate, "exp_up": exp_up, "exp_down": exp_down}


norm_eps = 1e-05

def normalize(tokens, norm_gain):
    values = tokens.astype(jnp.float32)
    factor = lax.rsqrt(lax.optimization_barrier(jnp.mean(values * values, axis=-1, keepdims=True)) + norm_eps)
    return (values * factor * norm_gain.astype(jnp.float32)).astype(jnp.bfloat16)

def count_slots(flat_ids, experts_all):
    onehot = (flat_ids[..., None] == jnp.arange(experts_all, dtype=jnp.int32)).astype(jnp.int32)
    before = jnp.cumsum(onehot, axis=1) - onehot
    return lax.optimization_barrier(jnp.sum(before * onehot, axis=-1)).astype(jnp.int32)

def reference(tokens, norm_gain, expert_ids, route_weight, exp_gate, exp_up, exp_down):
    devices_all = N_EP * N_TP
    normed = normalize(tokens, norm_gain)
    slots = count_slots(expert_ids.reshape(devices_all, TOK_DEV * TOPK), EXPERTS).reshape(TOKENS, TOPK)
    device_of = (jnp.arange(TOKENS, dtype=jnp.int32) // TOK_DEV)[:, None]
    where_buf = (device_of * CAP + slots).astype(jnp.int32)
    spare = devices_all * CAP
    block_ff = FF // N_TP

    def one_expert(mixed, inputs):
        index, w_gate, w_up, w_down = inputs
        chosen = expert_ids == index
        target = jnp.where(chosen, where_buf, spare).astype(jnp.int32)
        filled = jnp.zeros((spare + 1, D), jnp.bfloat16)
        for column in range(TOPK):
            filled = filled.at[target[:, column]].set(normed)
        filled = filled[:spare]
        gate = jnp.dot(filled, w_gate, preferred_element_type=jnp.float32)
        up_val = jnp.dot(filled, w_up, preferred_element_type=jnp.float32)
        hidden = (jax.nn.silu(gate) * up_val).astype(jnp.bfloat16)
        summed = jnp.zeros((spare, D), jnp.float32)
        for blockno in range(N_TP):
            part = jnp.dot(hidden[:, blockno * block_ff:(blockno + 1) * block_ff], w_down[blockno * block_ff:(blockno + 1) * block_ff], preferred_element_type=jnp.float32).astype(jnp.bfloat16)
            summed = summed + part.astype(jnp.float32)
        expert_out = summed.astype(jnp.bfloat16)
        safe = jnp.where(chosen, where_buf, 0).astype(jnp.int32)
        for column in range(TOPK):
            picked = expert_out[safe[:, column]].astype(jnp.float32)
            weight = jnp.where(chosen[:, column], route_weight[:, column], jnp.float32(0.0))
            mixed = mixed + weight[:, None] * picked
        return (mixed, None)
    start = jnp.zeros((TOKENS, D), jnp.float32)
    mixed, unused = lax.scan(one_expert, start, (jnp.arange(EXPERTS, dtype=jnp.int32), exp_gate, exp_up, exp_down))
    return mixed.astype(jnp.bfloat16)
```

```python
import jax
import jax.numpy as jnp
from jax import lax
from jax.experimental import pallas as pl
from jax.experimental.pallas import tpu as pltpu
from jax.sharding import PartitionSpec as P

TOP = 2
CAP = 10
EPS = 1e-05
Z, YC, TP = 4, 8, 4
PAIRS = CAP // 2
OFFSETS = (0, 1, 3, 2)
MESH = pl.DeviceIdType.MESH
BF16, F32 = jnp.bfloat16, jnp.float32


def kernel(
    ids_ref, weight_ref, tok_ref, gain_ref, gate_hbm, up_hbm, down_hbm, out_ref,
    w_gate, w_up, w_down, own_n, side_n, fill_o, fill_s, got, part, rows, hidden,
    ret_o, ret_s, back_o, back_s, rows_s, mix_out, mix_in,
    w_sem, pre_s, pre_r, yz_s, yz_r, xp_s, xp_r, xr_s, xr_r, yb_s, yb_r, fin_s, fin_r,
):
    me, x = lax.axis_index("ep"), lax.axis_index("tp")
    z, yc = me // YC, me % YC
    xr, xl, xo = (x + 1) % TP, (x + 3) % TP, (x + 2) % TP
    half = own_n.shape[2]
    toks = own_n.shape[1]
    side = (xl, xr)
    cols = (pl.ds(0, half), pl.ds(half, half))
    group = YC * CAP

    loads = [
        pltpu.make_async_copy(src.at[0], dst, w_sem.at[i])
        for i, (src, dst) in enumerate(((gate_hbm, w_gate), (up_hbm, w_up), (down_hbm, w_down)))
    ]
    for load in loads:
        load.start()

    barrier = pltpu.get_barrier_semaphore()

    @pl.loop(1, Z * YC)
    def _(i):
        pl.semaphore_signal(barrier, inc=1, device_id=((me + i) % (Z * YC), x), device_id_type=MESH)

    for peer in (xl, xr):
        pl.semaphore_signal(barrier, inc=1, device_id=(me, peer), device_id_type=MESH)

    def remote(src, dst, send, recv, ep, tp):
        return pltpu.make_async_remote_copy(
            src_ref=src, dst_ref=dst, send_sem=send, recv_sem=recv, device_id=(ep, tp), device_id_type=MESH
        )

    @pl.loop(0, toks // 32)
    def _(i):
        at = pl.ds(pl.multiple_of(i * 32, 32), 32)
        v = tok_ref[at, :].astype(F32)
        factor = lax.rsqrt(jnp.mean(v * v, axis=-1, keepdims=True) + EPS)
        n = (v * factor * gain_ref[...]).astype(BF16)
        own_n[0, at, :] = n[:, :half]
        own_n[1, at, :] = n[:, half:]

    pl.semaphore_wait(barrier, Z * YC - 1 + 2)
    pres = [
        remote(own_n.at[0], side_n.at[0], pre_s.at[0], pre_r.at[0], me, xr),
        remote(own_n.at[1], side_n.at[1], pre_s.at[1], pre_r.at[1], me, xl),
    ]
    for copy in pres:
        copy.start()

    def targets(at):
        pair = ids_ref[at]
        e = lax.broadcasted_iota(jnp.int32, (Z * YC, toks), 0)
        before = lax.broadcasted_iota(jnp.int32, (toks, toks), 0) < lax.broadcasted_iota(jnp.int32, (toks, toks), 1)
        named = [e == pair[k : k + 1, :] for k in range(TOP)]
        member = (named[0] | named[1]).astype(F32).astype(BF16)
        count = jnp.dot(member, before.astype(F32).astype(BF16), preferred_element_type=F32)
        slots = [jnp.sum(jnp.where(n, count, 0.0), axis=0, keepdims=True).astype(jnp.int32) for n in named]
        return [pair[k : k + 1, :] * CAP + slots[k] for k in range(TOP)]

    def pick(where, base):
        r = lax.broadcasted_iota(jnp.int32, (group, toks), 0) + base
        return ((r == where[0]) | (r == where[1])).astype(F32).astype(BF16)

    def filled(onehot, values):
        return jnp.dot(onehot, values, preferred_element_type=F32).astype(BF16).reshape(YC, PAIRS, 2, half)

    where_own = targets(x)
    for q in range(Z):
        ze = (z + Z - OFFSETS[q]) % Z
        onehot = pick(where_own, ze * group)
        for h in range(2):
            fill_o[ze, :, :, :, cols[h]] = filled(onehot, own_n[h])
        if q == 0:
            got[x, z, yc] = fill_o[z, yc]

        @pl.loop(1 if q == 0 else 0, YC)
        def _(i):
            j = (yc + i) % YC
            remote(fill_o.at[ze, j], got.at[x, z, yc], yz_s.at[0, q], yz_r.at[0, q], ze * YC + j, x).start()

    where_side = [targets(side[h]) for h in range(2)]
    for copy in pres:
        copy.wait()
    for q in range(Z):
        ze = (z + Z - OFFSETS[q]) % Z
        for h in range(2):
            fill_s[h, ze] = filled(pick(where_side[h], ze * group), side_n[h])
            if q == 0:
                got[side[h], z, yc, :, :, cols[h]] = fill_s[h, z, yc]

        @pl.loop(1 if q == 0 else 0, YC)
        def _(i):
            j = (yc + i) % YC
            for h in range(2):
                remote(
                    fill_s.at[h, ze, j], got.at[side[h], z, yc, :, :, cols[h]],
                    yz_s.at[1 + h, q], yz_r.at[1 + h, q], ze * YC + j, x,
                ).start()

    def source(q):
        return (z + OFFSETS[q]) % Z

    def posts(q):
        zs = source(q)
        plan = ((x, 0, xl), (x, 1, xr), (xl, 0, xr), (xr, 1, xl))
        return [
            remote(
                got.at[t, zs, :, :, :, cols[h]], got.at[t, zs, :, :, :, cols[h]],
                xp_s.at[k, q], xp_r.at[k, q], me, to,
            )
            for k, (t, h, to) in enumerate(plan)
        ]

    def drained(view, send, recv, q):
        count = YC - 1 if q == 0 else YC
        return remote(view.at[pl.ds(0, count)], view.at[pl.ds(0, count)], send, recv, me, xr)

    def forward(q):
        drained(fill_o.at[0], yz_s.at[0, q], yz_r.at[0, q], q).wait_recv()
        copies = posts(q)
        copies[0].start()
        copies[1].start()
        for h in range(2):
            drained(fill_s.at[h, 0], yz_s.at[1 + h, q], yz_r.at[1 + h, q], q).wait_recv()
            copies[2 + h].start()

    def returns(q):
        zs = source(q)
        return [
            remote(part.at[xr, zs, :, :, :, cols[0]], ret_o.at[zs, :, :, :, cols[0]], xr_s.at[0, q], xr_r.at[0, q], me, xr),
            remote(part.at[xo, zs, :, :, :, cols[0]], ret_s.at[0, zs], xr_s.at[1, q], xr_r.at[1, q], me, xl),
            remote(part.at[xl, zs, :, :, :, cols[1]], ret_o.at[zs, :, :, :, cols[1]], xr_s.at[2, q], xr_r.at[2, q], me, xl),
            remote(part.at[xo, zs, :, :, :, cols[1]], ret_s.at[1, zs], xr_s.at[3, q], xr_r.at[3, q], me, xr),
        ]

    def up_phase(q):
        zs = source(q)
        for t in range(TP):
            rows[pl.ds(t * group, group), :] = got[t, zs].reshape(group, 2 * half)
        if q == 0:
            loads[0].wait()
            loads[1].wait()

        @pl.loop(0, hidden.shape[1] // 256)
        def _(n):
            at = pl.ds(pl.multiple_of(n * 256, 256), 256)
            gate = jnp.dot(rows[...], w_gate[:, at], preferred_element_type=F32)
            up = jnp.dot(rows[...], w_up[:, at], preferred_element_type=F32)
            hidden[:, at] = (gate / (1.0 + jnp.exp(-gate)) * up).astype(BF16)

        if q == 0:
            loads[2].wait()

    def down_phase(q, h):
        zs = source(q)
        tiles = half // 256

        @pl.loop(h * tiles, (h + 1) * tiles)
        def _(n):
            at = pl.ds(pl.multiple_of(n * 256, 256), 256)
            o = jnp.dot(hidden[...], w_down[:, at], preferred_element_type=F32).astype(BF16)
            for t in range(TP):
                part[t, zs, :, :, :, at] = o[t * group : (t + 1) * group].reshape(YC, PAIRS, 2, 256)

    def give_back(q):
        zs = source(q)
        for copy in returns(q):
            copy.wait_recv()

        def summed(a, b):
            return (a.astype(F32) + b.astype(F32)).astype(BF16)

        @pl.loop(0, YC)
        def _(j):
            part[x, zs, j] = summed(part[x, zs, j], ret_o[zs, j])
            for h in range(2):
                part[side[h], zs, j, :, :, cols[h]] = summed(part[side[h], zs, j, :, :, cols[h]], ret_s[h, zs, j])

        if q == 0:
            back_o[z, yc] = part[x, z, yc]
            for h in range(2):
                back_s[h, z, yc] = part[side[h], z, yc, :, :, cols[h]]

        @pl.loop(1 if q == 0 else 0, YC)
        def _(i):
            j = (yc + i) % YC
            remote(part.at[x, zs, j], back_o.at[z, yc], yb_s.at[0, q], yb_r.at[0, q], zs * YC + j, x).start()
            for h in range(2):
                remote(
                    part.at[side[h], zs, j, :, :, cols[h]], back_s.at[h, z, yc],
                    yb_s.at[1 + h, q], yb_r.at[1 + h, q], zs * YC + j, x,
                ).start()

    forward(0)
    forward(1)
    for q in range(Z):
        for copy in posts(q):
            copy.wait_recv()
        up_phase(q)
        if q + 2 < Z:
            forward(q + 2)
        if q >= 1:
            give_back(q - 1)
        down_phase(q, 0)
        copies = returns(q)
        copies[0].start()
        copies[1].start()
        down_phase(q, 1)
        copies[2].start()
        copies[3].start()
    give_back(Z - 1)

    def spread(at, where):
        r = lax.broadcasted_iota(jnp.int32, (Z * group, toks), 0)
        w = weight_ref[at]
        full = jnp.where(r == where[0], w[0:1, :], 0.0) + jnp.where(r == where[1], w[1:2, :], 0.0)
        high = full.astype(BF16)
        return high, (full - high.astype(F32)).astype(BF16)

    def mixed(spreads, values):
        dims = (((0,), (0,)), ((), ()))
        return sum(lax.dot_general(s, values, dims, preferred_element_type=F32) for s in spreads)

    spreads = [spread(side[h], where_side[h]) for h in range(2)]
    finals = [
        remote(mix_out.at[0], mix_in.at[0], fin_s.at[0], fin_r.at[0], me, xl),
        remote(mix_out.at[1], mix_in.at[1], fin_s.at[1], fin_r.at[1], me, xr),
    ]
    for h in range(2):
        for q in range(Z):
            drained(fill_s.at[h, 0], yb_s.at[1 + h, q], yb_r.at[1 + h, q], q).wait_recv()
        for zz in range(Z):
            rows_s[h, pl.ds(zz * group, group), :] = back_s[h, zz].reshape(group, half)
        mix_out[h] = mixed(spreads[h], rows_s[h]).astype(BF16)
        finals[h].start()
    for q in range(Z):
        drained(fill_o.at[0], yb_s.at[0, q], yb_r.at[0, q], q).wait_recv()
    for zz in range(Z):
        rows[pl.ds(zz * group, group), :] = back_o[zz].reshape(group, 2 * half)
    spread_own = spread(x, where_own)
    for h in range(2):
        value = mixed(spread_own, rows[:, cols[h]])
        finals[h].wait()
        out_ref[:, cols[h]] = (value + mix_in[h].astype(F32)).astype(BF16)

    for q in range(Z):
        for copy in posts(q) + returns(q):
            copy.wait_send()
        for send in (yz_s, yb_s):
            for k, view in enumerate((fill_o.at[0], fill_s.at[0, 0], fill_s.at[1, 0])):
                drained(view, send.at[k, q], send.at[k, q], q).wait_send()


def per_device(tokens, norm_gain, expert_ids, route_weight, exp_gate, exp_up, exp_down):
    toks, width = tokens.shape
    half = width // 2
    inner = exp_gate.shape[2]
    ids = expert_ids.reshape(TP, toks, TOP).transpose(0, 2, 1)
    weight = route_weight.reshape(TP, toks, TOP).transpose(0, 2, 1)
    vmem, hbm = pl.BlockSpec(memory_space=pltpu.VMEM), pl.BlockSpec(memory_space=pl.ANY)
    dma = pltpu.SemaphoreType.DMA
    full, part = (YC, PAIRS, 2, width), (YC, PAIRS, 2, half)
    group = YC * CAP
    return pl.pallas_call(
        kernel,
        out_shape=jax.ShapeDtypeStruct((toks, width), BF16),
        in_specs=[vmem] * 4 + [hbm] * 3,
        out_specs=vmem,
        scratch_shapes=[
            pltpu.VMEM((width, inner), BF16),
            pltpu.VMEM((width, inner), BF16),
            pltpu.VMEM((inner, width), BF16),
            pltpu.VMEM((2, toks, half), BF16),
            pltpu.VMEM((2, toks, half), BF16),
            pltpu.VMEM((Z,) + full, BF16),
            pltpu.VMEM((2, Z) + part, BF16),
            pltpu.VMEM((TP, Z) + full, BF16),
            pltpu.VMEM((TP, Z) + full, BF16),
            pltpu.VMEM((TP * group, width), BF16),
            pltpu.VMEM((TP * group, inner), BF16),
            pltpu.VMEM((Z,) + full, BF16),
            pltpu.VMEM((2, Z) + part, BF16),
            pltpu.VMEM((Z,) + full, BF16),
            pltpu.VMEM((2, Z) + part, BF16),
            pltpu.VMEM((2, Z * group, half), BF16),
            pltpu.VMEM((2, toks, half), BF16),
            pltpu.VMEM((2, toks, half), BF16),
            dma((3,)),
            dma((2,)),
            dma((2,)),
            dma((3, Z)),
            dma((3, Z)),
            dma((4, Z)),
            dma((4, Z)),
            dma((4, Z)),
            dma((4, Z)),
            dma((3, Z)),
            dma((3, Z)),
            dma((2,)),
            dma((2,)),
        ],
        compiler_params=pltpu.CompilerParams(
            collective_id=0, has_side_effects=True, vmem_limit_bytes=63 * 2**20
        ),
    )(ids, weight, tokens, norm_gain.reshape(1, width), exp_gate, exp_up, exp_down)


def solution(mesh):
    return jax.shard_map(
        per_device,
        mesh=mesh,
        in_specs=(
            P(("ep", "tp"), None),
            P(),
            P("ep", None),
            P("ep", None),
            P("ep", None, "tp"),
            P("ep", None, "tp"),
            P("ep", "tp", None),
        ),
        out_specs=P(("ep", "tp"), None),
        check_vma=False,
    )
```

```python
import jax
import jax.numpy as jnp
from jax import lax
from jax.experimental import pallas as pl
from jax.experimental.pallas import tpu as pltpu
from jax.sharding import PartitionSpec as P

TOP = 2
CAP = 10
EPS = 1e-05
Z, YC, TP = 4, 8, 4
PAIRS = CAP // 2
ORDER = (1, 0, 3, 2)
MESH = pl.DeviceIdType.MESH
BF16, F32 = jnp.bfloat16, jnp.float32


def kernel(
    ids_ref, weight_ref, tok_ref, gain_ref, gate_hbm, up_hbm, down_hbm, out_ref,
    w_gate, w_up, w_down, own_n, side_n, fill_o, fill_s, got, part, rows, hidden,
    ret_o, ret_s, back_o, back_s, rows_s, mix_out, mix_in,
    w_sem, pre_s, pre_r, yz_s, yz_r, xp_s, xp_r, xr_s, xr_r, yb_s, yb_r, fin_s, fin_r,
):
    me, x = lax.axis_index("ep"), lax.axis_index("tp")
    z, y, core = me // 8, me // 2 % 4, me % 2
    xr, xl, xo = (x + 1) % TP, (x + 3) % TP, (x + 2) % TP
    half = own_n.shape[2]
    toks = own_n.shape[1]
    side = (xl, xr)
    cols = (pl.ds(0, half), pl.ds(half, half))
    group = YC * CAP

    loads = [
        pltpu.make_async_copy(src.at[0], dst, w_sem.at[i])
        for i, (src, dst) in enumerate(((gate_hbm, w_gate), (up_hbm, w_up), (down_hbm, w_down)))
    ]
    for load in loads:
        load.start()

    barrier = pltpu.get_barrier_semaphore()

    @pl.loop(1, Z * YC)
    def _(i):
        pl.semaphore_signal(barrier, inc=1, device_id=((me + i) % (Z * YC), x), device_id_type=MESH)

    for peer in (xl, xr):
        pl.semaphore_signal(barrier, inc=1, device_id=(me, peer), device_id_type=MESH)

    def remote(src, dst, send, recv, ep, tp):
        return pltpu.make_async_remote_copy(
            src_ref=src, dst_ref=dst, send_sem=send, recv_sem=recv, device_id=(ep, tp), device_id_type=MESH
        )

    @pl.loop(0, toks // 32)
    def _(i):
        at = pl.ds(pl.multiple_of(i * 32, 32), 32)
        v = tok_ref[at, :].astype(F32)
        factor = lax.rsqrt(jnp.mean(v * v, axis=-1, keepdims=True) + EPS)
        n = (v * factor * gain_ref[...]).astype(BF16)
        own_n[0, at, :] = n[:, :half]
        own_n[1, at, :] = n[:, half:]

    with jax.named_scope("bar"):
        pl.semaphore_wait(barrier, Z * YC - 1 + 2)
    pres = [
        remote(own_n.at[0], side_n.at[0], pre_s.at[0], pre_r.at[0], me, xr),
        remote(own_n.at[1], side_n.at[1], pre_s.at[1], pre_r.at[1], me, xl),
    ]
    for copy in pres:
        copy.start()

    def targets(at):
        pair = ids_ref[at]
        e = lax.broadcasted_iota(jnp.int32, (Z * YC, toks), 0)
        before = lax.broadcasted_iota(jnp.int32, (toks, toks), 0) < lax.broadcasted_iota(jnp.int32, (toks, toks), 1)
        named = [e == pair[k : k + 1, :] for k in range(TOP)]
        member = (named[0] | named[1]).astype(F32).astype(BF16)
        count = jnp.dot(member, before.astype(F32).astype(BF16), preferred_element_type=F32)
        slots = [jnp.sum(jnp.where(n, count, 0.0), axis=0, keepdims=True).astype(jnp.int32) for n in named]
        dz = (z - (pair >> 3)) & 3
        k = (y - (pair >> 1) - dz) & 3
        base = ((k * 4 + dz) * 2 + (pair & 1)) * CAP
        return [base[k : k + 1, :] + slots[k] for k in range(TOP)]

    def pick(where, base):
        r = lax.broadcasted_iota(jnp.int32, (group, toks), 0) + base
        return ((r == where[0]) | (r == where[1])).astype(F32).astype(BF16)

    def filled(onehot, values):
        return jnp.dot(onehot, values, preferred_element_type=F32).astype(BF16).reshape(YC, PAIRS, 2, half)

    def each(k, sign, send):
        @pl.loop(1 if k == 0 else 0, YC)
        def _(i):
            dz, c = i // 2, (core + i) % 2
            ep = (z + 4 + sign * dz) % 4 * 8 + (y + 8 + sign * (dz + k)) % 4 * 2 + c
            send(dz * 2 + c, dz * 2 + core, ep)

    def drained(view, send, recv, k):
        count = YC - 1 if k == 0 else YC
        return remote(view.at[pl.ds(0, count)], view.at[pl.ds(0, count)], send, recv, me, xr)

    where_own = targets(x)
    for k in ORDER:
        onehot = pick(where_own, k * group)
        for h in range(2):
            fill_o[k, :, :, :, cols[h]] = filled(onehot, own_n[h])
        if k == 0:
            got[x, k, core] = fill_o[k, core]

        def send_own(j, mine, ep):
            remote(fill_o.at[k, j], got.at[x, k, mine], yz_s.at[0, k], yz_r.at[0, k], ep, x).start()

        each(k, -1, send_own)

    def posts(k):
        plan = ((x, 0, xl), (x, 1, xr), (xl, 0, xr), (xr, 1, xl))
        return [
            remote(
                got.at[t, k, :, :, :, cols[h]], got.at[t, k, :, :, :, cols[h]],
                xp_s.at[i, k], xp_r.at[i, k], me, to,
            )
            for i, (t, h, to) in enumerate(plan)
        ]

    def forward_own(k):
        with jax.named_scope("fo"):
            drained(fill_o.at[0], yz_s.at[0, k], yz_r.at[0, k], k).wait_recv()
        for copy in posts(k)[:2]:
            copy.start()

    def forward_side(k):
        for h in range(2):
            with jax.named_scope("fs"):
                drained(fill_s.at[h, 0], yz_s.at[1 + h, k], yz_r.at[1 + h, k], k).wait_recv()
            posts(k)[2 + h].start()

    where_side = [targets(side[h]) for h in range(2)]
    forward_own(ORDER[0])
    with jax.named_scope("pre"):
        for copy in pres:
            copy.wait()
    for k in ORDER:
        for h in range(2):
            fill_s[h, k] = filled(pick(where_side[h], k * group), side_n[h])
            if k == 0:
                got[side[h], k, core, :, :, cols[h]] = fill_s[h, k, core]

        def send_side(j, mine, ep):
            for h in range(2):
                remote(
                    fill_s.at[h, k, j], got.at[side[h], k, mine, :, :, cols[h]],
                    yz_s.at[1 + h, k], yz_r.at[1 + h, k], ep, x,
                ).start()

        each(k, -1, send_side)
    for k in ORDER[1:]:
        forward_own(k)

    def splits(k):
        return 2 if k == ORDER[-1] else 1

    def cut(k, h, r):
        width = half // splits(k)
        return pl.ds(h * half + r * width, width)

    def inner(k, r):
        width = half // splits(k)
        return pl.ds(r * width, width)

    def slot(k, r):
        return ORDER.index(k) + r

    def returns(k, r):
        i = slot(k, r)
        plan = ((xr, 0, 0, xr), (xo, 0, 1, xl), (xl, 1, 0, xl), (xo, 1, 1, xr))
        out = []
        for n, (t, h, kind, to) in enumerate(plan):
            dst = ret_s.at[h, k, :, :, :, inner(k, r)] if kind else ret_o.at[k, :, :, :, cut(k, h, r)]
            out.append(remote(part.at[t, k, :, :, :, cut(k, h, r)], dst, xr_s.at[n, i], xr_r.at[n, i], me, to))
        return out

    def up_phase(blocks, first):
        size = len(blocks) * group
        for i, (t, k) in enumerate(blocks):
            rows[pl.ds(i * group, group), :] = got[t, k].reshape(group, 2 * half)
        if first:
            loads[0].wait()
            loads[1].wait()
        for n in range(hidden.shape[1] // 256):
            at = pl.ds(n * 256, 256)
            gate = jnp.dot(rows[:size, :], w_gate[:, at], preferred_element_type=F32)
            up = jnp.dot(rows[:size, :], w_up[:, at], preferred_element_type=F32)
            hidden[:size, at] = (gate / (1.0 + jnp.exp(-gate)) * up).astype(BF16)
        if first:
            loads[2].wait()

    def down_phase(blocks, at):
        size = len(blocks) * group
        o = jnp.dot(hidden[:size, :], w_down[:, at], preferred_element_type=F32).astype(BF16)
        for i, (t, k) in enumerate(blocks):
            part[t, k, :, :, :, at] = o[i * group : (i + 1) * group].reshape(YC, PAIRS, 2, at.size)

    def give_back(k, r):
        with jax.named_scope("gw"):
            for copy in returns(k, r):
                copy.wait_recv()
        with jax.named_scope("gs"):

            @pl.loop(0, YC)
            def _(j):
                for h in range(2):
                    at = cut(k, h, r)
                    part[x, k, j, :, :, at] = part[x, k, j, :, :, at] + ret_o[k, j, :, :, at]
                    part[side[h], k, j, :, :, at] = part[side[h], k, j, :, :, at] + ret_s[h, k, j, :, :, inner(k, r)]

        if k == 0:
            for h in range(2):
                at = cut(k, h, r)
                back_o[k, core, :, :, at] = part[x, k, core, :, :, at]
                back_s[h, k, core, :, :, inner(k, r)] = part[side[h], k, core, :, :, at]
        i = slot(k, r)

        def send_back(j, mine, ep):
            for h in range(2):
                remote(
                    part.at[side[h], k, j, :, :, cut(k, h, r)], back_s.at[h, k, mine, :, :, inner(k, r)],
                    yb_s.at[1 + h, i], yb_r.at[1 + h, i], ep, x,
                ).start()
            for h in range(2):
                at = cut(k, h, r)
                remote(
                    part.at[x, k, j, :, :, at], back_o.at[k, mine, :, :, at],
                    yb_s.at[0, i], yb_r.at[0, i], ep, x,
                ).start()

        each(k, 1, send_back)

    own = [(x, k) for k in ORDER]
    with jax.named_scope("up0"):
        up_phase(own, True)
    forward_side(ORDER[0])
    with jax.named_scope("down0"):
        for h in range(2):
            down_phase(own, pl.ds(h * half, half))
    forward_side(ORDER[1])
    for p, k in enumerate(ORDER):
        blocks = [(t, k) for t in (xl, xr, xo)]
        with jax.named_scope("pw"):
            for copy in posts(k):
                copy.wait_recv()
        with jax.named_scope("up"):
            up_phase(blocks, False)
        if p == 0:
            forward_side(ORDER[2])
        if p >= 2:
            give_back(ORDER[p - 2], 0)
        for r in range(splits(k)):
            with jax.named_scope("dn"):
                copies = returns(k, r)
                for h in range(2):
                    down_phase(blocks, cut(k, h, r))
                    copies[2 * h].start()
                    copies[2 * h + 1].start()
        if p == 0:
            forward_side(ORDER[3])
    give_back(ORDER[2], 0)
    give_back(ORDER[3], 0)
    give_back(ORDER[3], 1)

    def spread(at, where):
        r = lax.broadcasted_iota(jnp.int32, (Z * group, toks), 0)
        w = weight_ref[at]
        full = jnp.where(r == where[0], w[0:1, :], 0.0) + jnp.where(r == where[1], w[1:2, :], 0.0)
        high = full.astype(BF16)
        return high, (full - high.astype(F32)).astype(BF16)

    def mixed(spreads, values):
        dims = (((0,), (0,)), ((), ()))
        return sum(lax.dot_general(s, values, dims, preferred_element_type=F32) for s in spreads)

    last = ORDER[-1]
    spreads = [spread(side[h], where_side[h]) for h in range(2)]
    spread_own = spread(x, where_own)

    def back_side(h, k, r):
        view = fill_s.at[h, 0, :, :, :, inner(k, r)]
        return drained(view, yb_s.at[1 + h, slot(k, r)], yb_r.at[1 + h, slot(k, r)], k)

    def back_own(k, r):
        view = fill_s.at[0, 0] if splits(k) == 2 else fill_o.at[0]
        return drained(view, yb_s.at[0, slot(k, r)], yb_r.at[0, slot(k, r)], k)

    finals = {}
    for r in range(splits(last)):
        for h in range(2):
            with jax.named_scope("bs"):
                for k in ORDER:
                    if r < splits(k):
                        back_side(h, k, r).wait_recv()
            at = inner(last, r)
            for k in range(Z):
                rows_s[h, pl.ds(k * group, group), at] = back_s[h, k, :, :, :, at].reshape(group, at.size)
            mix_out[h, r] = mixed(spreads[h], rows_s[h, :, at]).astype(BF16)
            finals[h, r] = remote(mix_out.at[h, r], mix_in.at[h, r], fin_s.at[h, r], fin_r.at[h, r], me, side[h])
            finals[h, r].start()
    for r in range(splits(last)):
        with jax.named_scope("bo"):
            for k in ORDER:
                if r < splits(k):
                    back_own(k, r).wait_recv()
        for h in range(2):
            at = cut(last, h, r)
            for k in range(Z):
                rows[pl.ds(k * group, group), at] = back_o[k, :, :, :, at].reshape(group, at.size)
            value = mixed(spread_own, rows[:, at])
            with jax.named_scope("fin"):
                finals[h, r].wait()
            out_ref[:, at] = (value + mix_in[h, r].astype(F32)).astype(BF16)

    for k in ORDER:
        for copy in posts(k):
            copy.wait_send()
        for r in range(splits(k)):
            for copy in returns(k, r):
                copy.wait_send()
            back_own(k, r).wait_send()
            for h in range(2):
                back_side(h, k, r).wait_send()
        for i, view in enumerate((fill_o.at[0], fill_s.at[0, 0], fill_s.at[1, 0])):
            drained(view, yz_s.at[i, k], yz_s.at[i, k], k).wait_send()


def per_device(tokens, norm_gain, expert_ids, route_weight, exp_gate, exp_up, exp_down):
    toks, width = tokens.shape
    half = width // 2
    inner = exp_gate.shape[2]
    ids = expert_ids.reshape(TP, toks, TOP).transpose(0, 2, 1)
    weight = route_weight.reshape(TP, toks, TOP).transpose(0, 2, 1)
    vmem, hbm = pl.BlockSpec(memory_space=pltpu.VMEM), pl.BlockSpec(memory_space=pl.ANY)
    dma = pltpu.SemaphoreType.DMA
    full, part = (YC, PAIRS, 2, width), (YC, PAIRS, 2, half)
    group = YC * CAP
    return pl.pallas_call(
        kernel,
        out_shape=jax.ShapeDtypeStruct((toks, width), BF16),
        in_specs=[vmem] * 4 + [hbm] * 3,
        out_specs=vmem,
        scratch_shapes=[
            pltpu.VMEM((width, inner), BF16),
            pltpu.VMEM((width, inner), BF16),
            pltpu.VMEM((inner, width), BF16),
            pltpu.VMEM((2, toks, half), BF16),
            pltpu.VMEM((2, toks, half), BF16),
            pltpu.VMEM((Z,) + full, BF16),
            pltpu.VMEM((2, Z) + part, BF16),
            pltpu.VMEM((TP, Z) + full, BF16),
            pltpu.VMEM((TP, Z) + full, BF16),
            pltpu.VMEM((TP * group, width), BF16),
            pltpu.VMEM((TP * group, inner), BF16),
            pltpu.VMEM((Z,) + full, BF16),
            pltpu.VMEM((2, Z) + part, BF16),
            pltpu.VMEM((Z,) + full, BF16),
            pltpu.VMEM((2, Z) + part, BF16),
            pltpu.VMEM((2, Z * group, half), BF16),
            pltpu.VMEM((2, 2, toks, half // 2), BF16),
            pltpu.VMEM((2, 2, toks, half // 2), BF16),
            dma((3,)),
            dma((2,)),
            dma((2,)),
            dma((3, Z)),
            dma((3, Z)),
            dma((4, Z)),
            dma((4, Z)),
            dma((4, Z + 1)),
            dma((4, Z + 1)),
            dma((3, Z + 1)),
            dma((3, Z + 1)),
            dma((2, 2)),
            dma((2, 2)),
        ],
        compiler_params=pltpu.CompilerParams(
            collective_id=0, has_side_effects=True, vmem_limit_bytes=63 * 2**20
        ),
    )(ids, weight, tokens, norm_gain.reshape(1, width), exp_gate, exp_up, exp_down)


def solution(mesh):
    return jax.shard_map(
        per_device,
        mesh=mesh,
        in_specs=(
            P(("ep", "tp"), None),
            P(),
            P("ep", None),
            P("ep", None),
            P("ep", None, "tp"),
            P("ep", None, "tp"),
            P("ep", "tp", None),
        ),
        out_specs=P(("ep", "tp"), None),
        check_vma=False,
    )
```

```python
import jax
import jax.numpy as jnp
from jax import lax
from jax.experimental import pallas as pl
from jax.experimental.pallas import tpu as pltpu
from jax.sharding import PartitionSpec as P

TOP = 2
CAP = 10
EPS = 1e-05
Z, YC, TP = 4, 8, 4
PAIRS = CAP // 2
ORDER = (1, 0, 3, 2)
WIDE = 8
MESH = pl.DeviceIdType.MESH
BF16, F32 = jnp.bfloat16, jnp.float32


def kernel(
    ids_ref, weight_ref, gain_ref, tok_hbm, gate_hbm, up_hbm, down_hbm, out_ref,
    w_gate, w_up, w_down, tok, own_n, side_n, fill_o, fill_s, got, part, rows, hidden,
    ret_o, ret_s, back_o, back_s, rows_s, mix_out, mix_in, spreads,
    w_sem, pre_s, pre_r, yz_s, yz_r, xp_s, xp_r, xr_s, xr_r, yb_s, yb_r, fin_s, fin_r,
):
    me, x = lax.axis_index("ep"), lax.axis_index("tp")
    z, y, core = me // 8, me // 2 % 4, me % 2
    xr, xl, xo = (x + 1) % TP, (x + 3) % TP, (x + 2) % TP
    toks, full = own_n.shape
    wide = side_n.shape[2]
    half, rest, quarter = full // 2, full - wide, full // 4
    side = (xl, xr)
    group = YC * CAP
    tiles = hidden.shape[1] // 256

    barrier = pltpu.get_barrier_semaphore()

    @pl.loop(1, Z * YC)
    def _(i):
        pl.semaphore_signal(barrier, inc=1, device_id=((me + i) % (Z * YC), x), device_id_type=MESH)

    for peer in (xl, xr):
        pl.semaphore_signal(barrier, inc=1, device_id=(me, peer), device_id_type=MESH)

    sources = ((gate_hbm.at[0], w_gate), (up_hbm.at[0], w_up), (down_hbm.at[0], w_down), (tok_hbm, tok))
    loads = [pltpu.make_async_copy(src, dst, w_sem.at[i]) for i, (src, dst) in enumerate(sources)]
    loads[3].start()

    def remote(src, dst, send, recv, ep, tp):
        return pltpu.make_async_remote_copy(
            src_ref=src, dst_ref=dst, send_sem=send, recv_sem=recv, device_id=(ep, tp), device_id_type=MESH
        )

    def mirror(h, lo, hi):
        return (lo, hi) if h == 0 else (full - hi, full - lo)

    def cols(h, lo, hi, base=0):
        lo, hi = mirror(h, lo, hi)
        return pl.ds(lo - base, hi - lo)

    loads[3].wait()
    for load in loads[:3]:
        load.start()

    @pl.loop(0, toks // 32)
    def _(i):
        at = pl.ds(pl.multiple_of(i * 32, 32), 32)
        v = tok[at, :].astype(F32)
        factor = lax.rsqrt(jnp.mean(v * v, axis=-1, keepdims=True) + EPS)
        own_n[at, :] = (v * factor * gain_ref[...]).astype(BF16)

    with jax.named_scope("bar"):
        pl.semaphore_wait(barrier, Z * YC - 1 + 2)
    pres = [
        remote(own_n.at[:, cols(h, 0, wide)], side_n.at[h], pre_s.at[h], pre_r.at[h], me, (xr, xl)[h])
        for h in range(2)
    ]
    for copy in pres:
        copy.start()

    def targets(at):
        pair = ids_ref[at]
        e = lax.broadcasted_iota(jnp.int32, (Z * YC, toks), 0)
        before = lax.broadcasted_iota(jnp.int32, (toks, toks), 0) < lax.broadcasted_iota(jnp.int32, (toks, toks), 1)
        named = [e == pair[k : k + 1, :] for k in range(TOP)]
        member = (named[0] | named[1]).astype(F32).astype(BF16)
        count = jnp.dot(member, before.astype(F32).astype(BF16), preferred_element_type=F32)
        slots = [jnp.sum(jnp.where(n, count, 0.0), axis=0, keepdims=True).astype(jnp.int32) for n in named]
        dz = (z - (pair >> 3)) & 3
        k = (y - (pair >> 1) - dz) & 3
        base = ((k * 4 + dz) * 2 + (pair & 1)) * CAP
        return [base[k : k + 1, :] + slots[k] for k in range(TOP)]

    def pick(where, base):
        r = lax.broadcasted_iota(jnp.int32, (group, toks), 0) + base
        return ((r == where[0]) | (r == where[1])).astype(F32).astype(BF16)

    def filled(onehot, values):
        o = jnp.dot(onehot, values, preferred_element_type=F32).astype(BF16)
        return o.reshape(YC, PAIRS, 2, values.shape[1])

    def each(k, sign, send):
        @pl.loop(1 if k == 0 else 0, YC)
        def _(i):
            dz, c = i // 2, (core + i) % 2
            ep = (z + 4 + sign * dz) % 4 * 8 + (y + 8 + sign * (dz + k)) % 4 * 2 + c
            send(dz * 2 + c, dz * 2 + core, ep)

    def drained(view, send, recv, k):
        count = YC - 1 if k == 0 else YC
        return remote(view.at[pl.ds(0, count)], view.at[pl.ds(0, count)], send, recv, me, xr)

    where_own = targets(x)

    def fill_own(k):
        fill_o[k] = filled(pick(where_own, k * group), own_n[...])
        if k == 0:
            got[x, k, core] = fill_o[k, core]

    def send_own(k):
        def send(j, mine, ep):
            remote(fill_o.at[k, j], got.at[x, k, mine], yz_s.at[0, k], yz_r.at[0, k], ep, x).start()

        each(k, -1, send)

    def fill_side(k):
        for h in range(2):
            fill_s[h, k] = filled(pick(where_side[h], k * group), side_n[h])
            if k == 0:
                got[side[h], k, core, :, :, cols(h, 0, wide)] = fill_s[h, k, core]

    def send_side(k):
        def send(j, mine, ep):
            for h in range(2):
                remote(
                    fill_s.at[h, k, j], got.at[side[h], k, mine, :, :, cols(h, 0, wide)],
                    yz_s.at[1 + h, k], yz_r.at[1 + h, k], ep, x,
                ).start()

        each(k, -1, send)

    def post(k, i):
        t, h, to = ((x, 0, xl), (x, 1, xr), (xl, 0, xr), (xr, 1, xl))[i]
        at = cols(h, 0, half if i >= 2 else rest)
        ref = got.at[t, k, :, :, :, at]
        return remote(ref, ref, xp_s.at[i, k], xp_r.at[i, k], me, to)

    def forward_own(k):
        with jax.named_scope("fo"):
            drained(fill_o.at[0], yz_s.at[0, k], yz_r.at[0, k], k).wait_recv()
        for i in range(2):
            post(k, i).start()

    def forward_side(k):
        for h in range(2):
            with jax.named_scope("fs"):
                drained(fill_s.at[h, 0], yz_s.at[1 + h, k], yz_r.at[1 + h, k], k).wait_recv()
            post(k, 2 + h).start()

    k0, k1, k2, k3 = ORDER
    for k in ORDER:
        fill_own(k)
        send_own(k)
    where_side = [targets(side[h]) for h in range(2)]
    forward_own(k0)
    with jax.named_scope("pre"):
        for copy in pres:
            copy.wait()
    for k in ORDER:
        fill_side(k)
        send_side(k)
    forward_own(k1)

    for i, (at, where) in enumerate(((xl, where_side[0]), (xr, where_side[1]), (x, where_own))):
        r = lax.broadcasted_iota(jnp.int32, (Z * group, toks), 0)
        w = weight_ref[at]
        exact = jnp.where(r == where[0], w[0:1, :], 0.0) + jnp.where(r == where[1], w[1:2, :], 0.0)
        high = exact.astype(BF16)
        spreads[i, 0] = high
        spreads[i, 1] = (exact - high.astype(F32)).astype(BF16)

    forward_own(k2)
    forward_own(k3)

    def span(r):
        return ((0, quarter), (quarter, wide))[r]

    def own_spans(r):
        return [(0, quarter), (full - quarter, full)] if r == 0 else [(quarter, full - quarter)]

    def slot(k, r):
        return 2 * k + r

    def returns(k, r):
        i = slot(k, r)
        lo, hi = span(r)
        out = []
        for h in range(2):
            at = cols(h, lo, min(hi, rest))
            near, far = ((xr, xl), (xl, xr))[h]
            out.append(remote(part.at[near, k, :, :, :, at], ret_o.at[k, :, :, :, at], xr_s.at[2 * h, i], xr_r.at[2 * h, i], me, near))
            at, inner = cols(h, lo, min(hi, half)), cols(h, lo, min(hi, half), h * half)
            out.append(remote(part.at[xo, k, :, :, :, at], ret_s.at[h, k, :, :, :, inner], xr_s.at[2 * h + 1, i], xr_r.at[2 * h + 1, i], me, far))
        return out

    def up_phase(blocks, first, services):
        size = len(blocks) * group
        for i, (t, k) in enumerate(blocks):
            rows[pl.ds(i * group, group), :] = got[t, k].reshape(group, full)
        if first:
            loads[0].wait()
            loads[1].wait()
        for n in range(tiles):
            at = pl.ds(n * 256, 256)
            gate = jnp.dot(rows[:size, :], w_gate[:, at], preferred_element_type=F32)
            up = jnp.dot(rows[:size, :], w_up[:, at], preferred_element_type=F32)
            hidden[:size, at] = (gate / (1.0 + jnp.exp(-gate)) * up).astype(BF16)
            if n in services:
                services[n]()
        if first:
            loads[2].wait()

    def down_phase(blocks, lo, hi):
        size = len(blocks) * group
        at = pl.ds(lo, hi - lo)
        o = jnp.dot(hidden[:size, :], w_down[:, at], preferred_element_type=F32).astype(BF16)
        for i, (t, k) in enumerate(blocks):
            part[t, k, :, :, :, at] = o[i * group : (i + 1) * group].reshape(YC, PAIRS, 2, hi - lo)

    def give_back(k, r):
        lo, hi = span(r)
        with jax.named_scope("gw"):
            for copy in returns(k, r):
                copy.wait_recv()
        with jax.named_scope("gs"):

            @pl.loop(0, YC)
            def _(j):
                for h in range(2):
                    at = cols(h, lo, min(hi, rest))
                    part[x, k, j, :, :, at] = part[x, k, j, :, :, at] + ret_o[k, j, :, :, at]
                    at, inner = cols(h, lo, min(hi, half)), cols(h, lo, min(hi, half), h * half)
                    part[side[h], k, j, :, :, at] = part[side[h], k, j, :, :, at] + ret_s[h, k, j, :, :, inner]

        i = slot(k, r)
        views = [(part.at[side[h]], back_s.at[h], cols(h, lo, hi), cols(h, lo, hi, h * rest), 1 + h) for h in range(2)]
        views += [(part.at[x], back_o, pl.ds(a, b - a), pl.ds(a, b - a), 0) for a, b in own_spans(r)]
        if k == 0:
            for src, dst, at, inner, _ in views:
                dst[k, core, :, :, inner] = src[k, core, :, :, at]

        def send(j, mine, ep):
            for src, dst, at, inner, n in views:
                remote(src.at[k, j, :, :, at], dst.at[k, mine, :, :, inner], yb_s.at[n, i], yb_r.at[n, i], ep, x).start()

        each(k, 1, send)

    def chunk(k, services):
        blocks = [(t, k) for t in (xl, xr, xo)]
        with jax.named_scope("pw"):
            for i in range(4):
                post(k, i).wait_recv()
        with jax.named_scope("up"):
            up_phase(blocks, False, services)
        for r in range(2):
            with jax.named_scope("dn"):
                for lo, hi in own_spans(r):
                    down_phase(blocks, lo, hi)
            for copy in returns(k, r):
                copy.start()

    own = [(x, k) for k in ORDER]
    with jax.named_scope("upo"):
        up_phase(own, True, {3: lambda: forward_side(k0), 6: lambda: forward_side(k1)})
    with jax.named_scope("dno"):
        down_phase(own, 0, half)
        down_phase(own, half, full)
    chunk(k0, {2: lambda: forward_side(k2)})
    forward_side(k3)
    chunk(k1, {6: lambda: give_back(k0, 0)})
    chunk(k2, {0: lambda: give_back(k0, 1)})
    chunk(k3, {1: lambda: give_back(k1, 0), 6: lambda: give_back(k1, 1)})
    for k in (k2, k3):
        for r in range(2):
            give_back(k, r)

    def mixed(i, values):
        dims = (((0,), (0,)), ((), ()))
        return sum(lax.dot_general(spreads[i, n], values, dims, preferred_element_type=F32) for n in range(2))

    def back_side(h, k, r):
        lo, hi = span(r)
        view = fill_s.at[h, 0, :, :, :, pl.ds(0, hi - lo)]
        return drained(view, yb_s.at[1 + h, slot(k, r)], yb_r.at[1 + h, slot(k, r)], k)

    def back_own(k, r):
        view = fill_o.at[0, :, :, :, pl.ds(0, half)]
        return drained(view, yb_s.at[0, slot(k, r)], yb_r.at[0, slot(k, r)], k)

    finals = {}
    for r in range(2):
        lo, hi = span(r)
        for h in range(2):
            with jax.named_scope("bs"):
                for k in ORDER:
                    back_side(h, k, r).wait_recv()
            at = cols(h, lo, hi, h * rest)
            for k in range(Z):
                rows_s[h, pl.ds(k * group, group), at] = back_s[h, k, :, :, :, at].reshape(group, hi - lo)
            mix_out[h, :, at] = mixed(h, rows_s[h, :, at]).astype(BF16)
            finals[h, r] = remote(mix_out.at[h, :, at], mix_in.at[h, :, at], fin_s.at[h, r], fin_r.at[h, r], me, side[h])
            finals[h, r].start()
    for r in range(2):
        with jax.named_scope("bo"):
            for k in ORDER:
                back_own(k, r).wait_recv()
        for lo, hi in own_spans(r):
            at = pl.ds(lo, hi - lo)
            for k in range(Z):
                rows[pl.ds(k * group, group), at] = back_o[k, :, :, :, at].reshape(group, hi - lo)
        with jax.named_scope("fin"):
            for h in range(2):
                finals[h, r].wait()
        edges = sorted({e for lo, hi in own_spans(r) for e in (lo, hi)} | ({rest, wide} if r == 1 else set()))
        for lo, hi in zip(edges, edges[1:]):
            if r == 0 and lo == quarter:
                continue
            value = mixed(2, rows[:, lo:hi])
            if hi <= wide:
                value = value + mix_in[0, :, lo:hi].astype(F32)
            if lo >= rest:
                value = value + mix_in[1, :, lo - rest : hi - rest].astype(F32)
            out_ref[:, lo:hi] = value.astype(BF16)

    for k in ORDER:
        for i in range(4):
            post(k, i).wait_send()
        for r in range(2):
            for copy in returns(k, r):
                copy.wait_send()
            back_own(k, r).wait_send()
            for h in range(2):
                back_side(h, k, r).wait_send()
        for i, view in enumerate((fill_o.at[0], fill_s.at[0, 0], fill_s.at[1, 0])):
            drained(view, yz_s.at[i, k], yz_s.at[i, k], k).wait_send()


def per_device(tokens, norm_gain, expert_ids, route_weight, exp_gate, exp_up, exp_down):
    toks, width = tokens.shape
    half = width // 2
    wide = WIDE * width // 16
    inner = exp_gate.shape[2]
    ids = expert_ids.reshape(TP, toks, TOP).transpose(0, 2, 1)
    weight = route_weight.reshape(TP, toks, TOP).transpose(0, 2, 1)
    vmem, hbm = pl.BlockSpec(memory_space=pltpu.VMEM), pl.BlockSpec(memory_space=pl.ANY)
    dma = pltpu.SemaphoreType.DMA
    group = YC * CAP

    def copies(*lead, size=width):
        return pltpu.VMEM(lead + (YC, PAIRS, 2, size), BF16)

    return pl.pallas_call(
        kernel,
        out_shape=pltpu.VMEM((toks, width), BF16),
        in_specs=[vmem] * 3 + [hbm] * 4,
        out_specs=vmem,
        scratch_shapes=[
            pltpu.VMEM((width, inner), BF16),
            pltpu.VMEM((width, inner), BF16),
            pltpu.VMEM((inner, width), BF16),
            pltpu.VMEM((toks, width), BF16),
            pltpu.VMEM((toks, width), BF16),
            pltpu.VMEM((2, toks, wide), BF16),
            copies(Z),
            copies(2, Z, size=wide),
            copies(TP, Z),
            copies(TP, Z),
            pltpu.VMEM((TP * group, width), BF16),
            pltpu.VMEM((TP * group, inner), BF16),
            copies(Z),
            copies(2, Z, size=half),
            copies(Z),
            copies(2, Z, size=wide),
            pltpu.VMEM((2, Z * group, wide), BF16),
            pltpu.VMEM((2, toks, wide), BF16),
            pltpu.VMEM((2, toks, wide), BF16),
            pltpu.VMEM((3, 2, Z * group, toks), BF16),
            dma((4,)),
            dma((2,)),
            dma((2,)),
            dma((3, Z)),
            dma((3, Z)),
            dma((4, Z)),
            dma((4, Z)),
            dma((4, 2 * Z)),
            dma((4, 2 * Z)),
            dma((3, 2 * Z)),
            dma((3, 2 * Z)),
            dma((2, 2)),
            dma((2, 2)),
        ],
        compiler_params=pltpu.CompilerParams(
            collective_id=0, has_side_effects=True, vmem_limit_bytes=63 * 2**20
        ),
    )(ids, weight, norm_gain.reshape(1, width), tokens, exp_gate, exp_up, exp_down)


def solution(mesh):
    return jax.shard_map(
        per_device,
        mesh=mesh,
        in_specs=(
            P(("ep", "tp"), None),
            P(),
            P("ep", None),
            P("ep", None),
            P("ep", None, "tp"),
            P("ep", None, "tp"),
            P("ep", "tp", None),
        ),
        out_specs=P(("ep", "tp"), None),
        check_vma=False,
    )
```

```python
import jax
import jax.numpy as jnp
from jax import lax
from jax.experimental import pallas as pl
from jax.experimental.pallas import tpu as pltpu
from jax.sharding import PartitionSpec as P

TOP = 2
CAP = 10
EPS = 1e-05
Z, YC, TP = 4, 8, 4
PAIRS = CAP // 2
ORDER = (1, 0, 3, 2)
WIDE = 8
CUTS = (0, 4)
MESH = pl.DeviceIdType.MESH
BF16, F32 = jnp.bfloat16, jnp.float32


def kernel(
    ids_ref, weight_ref, gain_ref, tok_hbm, gate_hbm, up_hbm, down_hbm, out_ref,
    w_gate, w_up, w_down, tok, own_n, side_n, fill_o, fill_s, got, part, rows, hidden,
    ret_o, ret_s, back_o, back_s, rows_s, mix_out, mix_in, spreads, own_mix,
    w_sem, pre_s, pre_r, yz_s, yz_r, xp_s, xp_r, xr_s, xr_r, yb_s, yb_r, fin_s, fin_r,
):
    me, x = lax.axis_index("ep"), lax.axis_index("tp")
    z, y, core = me // 8, me // 2 % 4, me % 2
    xr, xl, xo = (x + 1) % TP, (x + 3) % TP, (x + 2) % TP
    toks, full = own_n.shape
    wide = side_n.shape[2]
    half, rest = full // 2, full - wide
    side = (xl, xr)
    group = YC * CAP
    tiles = hidden.shape[1] // 256

    barrier = pltpu.get_barrier_semaphore()

    @pl.loop(1, Z * YC)
    def _(i):
        pl.semaphore_signal(barrier, inc=1, device_id=((me + i) % (Z * YC), x), device_id_type=MESH)

    for peer in (xl, xr):
        pl.semaphore_signal(barrier, inc=1, device_id=(me, peer), device_id_type=MESH)

    sources = ((gate_hbm.at[0], w_gate), (up_hbm.at[0], w_up), (down_hbm.at[0], w_down), (tok_hbm, tok))
    loads = [pltpu.make_async_copy(src, dst, w_sem.at[i]) for i, (src, dst) in enumerate(sources)]
    loads[3].start()

    def remote(src, dst, send, recv, ep, tp):
        return pltpu.make_async_remote_copy(
            src_ref=src, dst_ref=dst, send_sem=send, recv_sem=recv, device_id=(ep, tp), device_id_type=MESH
        )

    def mirror(h, lo, hi):
        return (lo, hi) if h == 0 else (full - hi, full - lo)

    def cols(h, lo, hi, base=0):
        lo, hi = mirror(h, lo, hi)
        return pl.ds(lo - base, hi - lo)

    loads[3].wait()
    for load in loads[:3]:
        load.start()

    @pl.loop(0, toks // 32)
    def _(i):
        at = pl.ds(pl.multiple_of(i * 32, 32), 32)
        v = tok[at, :].astype(F32)
        factor = lax.rsqrt(jnp.mean(v * v, axis=-1, keepdims=True) + EPS)
        own_n[at, :] = (v * factor * gain_ref[...]).astype(BF16)

    with jax.named_scope("bar"):
        pl.semaphore_wait(barrier, Z * YC - 1 + 2)
    pres = [
        remote(own_n.at[:, cols(h, 0, wide)], side_n.at[h], pre_s.at[h], pre_r.at[h], me, (xr, xl)[h])
        for h in range(2)
    ]
    for copy in pres:
        copy.start()

    def targets(at):
        pair = ids_ref[at]
        e = lax.broadcasted_iota(jnp.int32, (Z * YC, toks), 0)
        before = lax.broadcasted_iota(jnp.int32, (toks, toks), 0) < lax.broadcasted_iota(jnp.int32, (toks, toks), 1)
        named = [e == pair[k : k + 1, :] for k in range(TOP)]
        member = (named[0] | named[1]).astype(F32).astype(BF16)
        count = jnp.dot(member, before.astype(F32).astype(BF16), preferred_element_type=F32)
        slots = [jnp.sum(jnp.where(n, count, 0.0), axis=0, keepdims=True).astype(jnp.int32) for n in named]
        dz = (z - (pair >> 3)) & 3
        k = (y - (pair >> 1) - dz) & 3
        base = ((k * 4 + dz) * 2 + (pair & 1)) * CAP
        return [base[k : k + 1, :] + slots[k] for k in range(TOP)]

    def pick(where, base):
        r = lax.broadcasted_iota(jnp.int32, (group, toks), 0) + base
        return ((r == where[0]) | (r == where[1])).astype(F32).astype(BF16)

    def filled(onehot, values):
        o = jnp.dot(onehot, values, preferred_element_type=F32).astype(BF16)
        return o.reshape(YC, PAIRS, 2, values.shape[1])

    def each(k, sign, send):
        @pl.loop(1 if k == 0 else 0, YC)
        def _(i):
            dz, c = i // 2, (core + i) % 2
            ep = (z + 4 + sign * dz) % 4 * 8 + (y + 8 + sign * (dz + k)) % 4 * 2 + c
            send(dz * 2 + c, dz * 2 + core, ep)

    def drained(view, send, recv, k):
        count = YC - 1 if k == 0 else YC
        return remote(view.at[pl.ds(0, count)], view.at[pl.ds(0, count)], send, recv, me, xr)

    where_own = targets(x)

    def fill_own(k):
        fill_o[k] = filled(pick(where_own, k * group), own_n[...])
        if k == 0:
            got[x, k, core] = fill_o[k, core]

    def send_own(k):
        def send(j, mine, ep):
            remote(fill_o.at[k, j], got.at[x, k, mine], yz_s.at[0, k], yz_r.at[0, k], ep, x).start()

        each(k, -1, send)

    def fill_side(k):
        for h in range(2):
            fill_s[h, k] = filled(pick(where_side[h], k * group), side_n[h])
            if k == 0:
                got[side[h], k, core, :, :, cols(h, 0, wide)] = fill_s[h, k, core]

    def send_side(k):
        def send(j, mine, ep):
            for h in range(2):
                remote(
                    fill_s.at[h, k, j], got.at[side[h], k, mine, :, :, cols(h, 0, wide)],
                    yz_s.at[1 + h, k], yz_r.at[1 + h, k], ep, x,
                ).start()

        each(k, -1, send)

    def post(k, i):
        t, h, to = ((x, 0, xl), (x, 1, xr), (xl, 0, xr), (xr, 1, xl))[i]
        at = cols(h, 0, half if i >= 2 else rest)
        ref = got.at[t, k, :, :, :, at]
        return remote(ref, ref, xp_s.at[i, k], xp_r.at[i, k], me, to)

    def forward_own(k):
        with jax.named_scope("fo"):
            drained(fill_o.at[0], yz_s.at[0, k], yz_r.at[0, k], k).wait_recv()
        for i in range(2):
            post(k, i).start()

    def forward_side(k):
        for h in range(2):
            with jax.named_scope("fs"):
                drained(fill_s.at[h, 0], yz_s.at[1 + h, k], yz_r.at[1 + h, k], k).wait_recv()
            post(k, 2 + h).start()

    k0, k1, k2, k3 = ORDER
    for k in ORDER:
        fill_own(k)
        send_own(k)
    where_side = [targets(side[h]) for h in range(2)]
    forward_own(k0)
    with jax.named_scope("pre"):
        for copy in pres:
            copy.wait()
    for k in ORDER:
        fill_side(k)
        send_side(k)
    forward_own(k1)

    for i, (at, where) in enumerate(((xl, where_side[0]), (xr, where_side[1]), (x, where_own))):
        r = lax.broadcasted_iota(jnp.int32, (Z * group, toks), 0)
        w = weight_ref[at]
        exact = jnp.where(r == where[0], w[0:1, :], 0.0) + jnp.where(r == where[1], w[1:2, :], 0.0)
        high = exact.astype(BF16)
        spreads[i, 0] = high
        spreads[i, 1] = (exact - high.astype(F32)).astype(BF16)

    forward_own(k2)
    forward_own(k3)

    bounds = [c * full // 16 for c in CUTS] + [wide]
    turns = len(CUTS)

    def span(r):
        return bounds[r], bounds[r + 1]

    def own_spans(r):
        lo, hi = span(r)
        return [(lo, full - lo)] if r == turns - 1 else [(lo, hi), (full - hi, full - lo)]

    def slot(k, r):
        return turns * k + r

    def returns(k, r):
        i = slot(k, r)
        lo, hi = span(r)
        out = []
        for h in range(2):
            at = cols(h, lo, min(hi, rest))
            near, far = ((xr, xl), (xl, xr))[h]
            out.append(remote(part.at[near, k, :, :, :, at], ret_o.at[k, :, :, :, at], xr_s.at[2 * h, i], xr_r.at[2 * h, i], me, near))
            at, inner = cols(h, lo, min(hi, half)), cols(h, lo, min(hi, half), h * half)
            out.append(remote(part.at[xo, k, :, :, :, at], ret_s.at[h, k, :, :, :, inner], xr_s.at[2 * h + 1, i], xr_r.at[2 * h + 1, i], me, far))
        return out

    def up_phase(blocks, first, services):
        size = len(blocks) * group
        for i, (t, k) in enumerate(blocks):
            rows[pl.ds(i * group, group), :] = got[t, k].reshape(group, full)
        if first:
            loads[0].wait()
            loads[1].wait()
        for n in range(tiles):
            at = pl.ds(n * 256, 256)
            gate = jnp.dot(rows[:size, :], w_gate[:, at], preferred_element_type=F32)
            up = jnp.dot(rows[:size, :], w_up[:, at], preferred_element_type=F32)
            hidden[:size, at] = (gate / (1.0 + jnp.exp(-gate)) * up).astype(BF16)
            if n in services:
                services[n]()
        if first:
            loads[2].wait()

    def down_phase(blocks, lo, hi):
        size = len(blocks) * group
        at = pl.ds(lo, hi - lo)
        o = jnp.dot(hidden[:size, :], w_down[:, at], preferred_element_type=F32).astype(BF16)
        for i, (t, k) in enumerate(blocks):
            part[t, k, :, :, :, at] = o[i * group : (i + 1) * group].reshape(YC, PAIRS, 2, hi - lo)

    def send_views(k, r, views):
        i = slot(k, r)
        if k == 0:
            for src, dst, at, inner, _ in views:
                dst[k, core, :, :, inner] = src[k, core, :, :, at]

        def send(j, mine, ep):
            for src, dst, at, inner, n in views:
                remote(src.at[k, j, :, :, at], dst.at[k, mine, :, :, inner], yb_s.at[n, i], yb_r.at[n, i], ep, x).start()

        each(k, 1, send)

    def side_sum(k, r, j):
        lo, hi = span(r)
        for h in range(2):
            at, inner = cols(h, lo, min(hi, half)), cols(h, lo, min(hi, half), h * half)
            part[side[h], k, j, :, :, at] = part[side[h], k, j, :, :, at] + ret_s[h, k, j, :, :, inner]

    def own_sum(k, r, j):
        lo, hi = span(r)
        for h in range(2):
            at = cols(h, lo, min(hi, rest))
            part[x, k, j, :, :, at] = part[x, k, j, :, :, at] + ret_o[k, j, :, :, at]

    def side_views(r):
        lo, hi = span(r)
        return [(part.at[side[h]], back_s.at[h], cols(h, lo, hi), cols(h, lo, hi, h * rest), 1 + h) for h in range(2)]

    def own_views(r):
        return [(part.at[x], back_o, pl.ds(a, b - a), pl.ds(a, b - a), 0) for a, b in own_spans(r)]

    def give_back(k, r, which=("side", "own")):
        with jax.named_scope("gw"):
            copies = returns(k, r)
            for copy in (copies[1::2] if "side" in which else []) + (copies[::2] if "own" in which else []):
                copy.wait_recv()
        with jax.named_scope("gs"):

            @pl.loop(0, YC)
            def _(j):
                if "side" in which:
                    side_sum(k, r, j)
                if "own" in which:
                    own_sum(k, r, j)

        send_views(k, r, (side_views(r) if "side" in which else []) + (own_views(r) if "own" in which else []))

    def chunk(k, services):
        blocks = [(t, k) for t in (xl, xr, xo)]
        with jax.named_scope("pw"):
            for i in range(4):
                post(k, i).wait_recv()
        with jax.named_scope("up"):
            up_phase(blocks, False, services)
        for r in range(turns):
            with jax.named_scope("dn"):
                for lo, hi in own_spans(r):
                    down_phase(blocks, lo, hi)
            copies = returns(k, r)
            for copy in copies[1::2] + (copies[::2] if k != k3 else []):
                copy.start()
        if k == k3:
            for r in range(turns):
                for copy in returns(k, r)[::2]:
                    copy.start()

    own = [(x, k) for k in ORDER]
    with jax.named_scope("upo"):
        up_phase(own, True, {3: lambda: forward_side(k0), 6: lambda: forward_side(k1)})
    with jax.named_scope("dno"):
        down_phase(own, 0, half)
        down_phase(own, half, full)
    chunk(k0, {2: lambda: forward_side(k2)})
    forward_side(k3)
    def give(k, *which):
        for r in which:
            give_back(k, r)

    later = range(1, turns)
    chunk(k1, {6: lambda: give(k0, 0)})
    chunk(k2, {0: lambda: give(k0, *later)})
    chunk(k3, {1: lambda: give(k1, 0), 6: lambda: give(k1, *later)})
    give(k2, *range(turns - 1))
    tail = ((k2, turns - 1), *((k3, r) for r in range(turns)))
    for which in ("side", "own"):
        for k, r in tail:
            give_back(k, r, (which,))

    def mixed(i, values):
        dims = (((0,), (0,)), ((), ()))
        return sum(lax.dot_general(spreads[i, n], values, dims, preferred_element_type=F32) for n in range(2))

    def back_side(h, k, r):
        lo, hi = span(r)
        view = fill_s.at[h, 0, :, :, :, pl.ds(0, hi - lo)]
        return drained(view, yb_s.at[1 + h, slot(k, r)], yb_r.at[1 + h, slot(k, r)], k)

    def back_own(k, r):
        view = fill_o.at[0, :, :, :, pl.ds(0, sum(hi - lo for lo, hi in own_spans(r)))]
        return drained(view, yb_s.at[0, slot(k, r)], yb_r.at[0, slot(k, r)], k)

    finals = {}
    for r in range(turns):
        lo, hi = span(r)
        for h in range(2):
            with jax.named_scope("bs"):
                for k in ORDER:
                    back_side(h, k, r).wait_recv()
            at = cols(h, lo, hi, h * rest)
            for k in range(Z):
                rows_s[h, pl.ds(k * group, group), at] = back_s[h, k, :, :, :, at].reshape(group, hi - lo)
            mix_out[h, :, at] = mixed(h, rows_s[h, :, at]).astype(BF16)
            finals[h, r] = remote(mix_out.at[h, :, at], mix_in.at[h, :, at], fin_s.at[h, r], fin_r.at[h, r], me, side[h])
            finals[h, r].start()
    for r in range(turns):
        with jax.named_scope("bo"):
            for k in ORDER:
                back_own(k, r).wait_recv()
        for lo, hi in own_spans(r):
            at = pl.ds(lo, hi - lo)
            for k in range(Z):
                rows[pl.ds(k * group, group), at] = back_o[k, :, :, :, at].reshape(group, hi - lo)
            own_mix[:, at] = mixed(2, rows[:, at])
    for r in range(turns):
        with jax.named_scope("fin"):
            for h in range(2):
                finals[h, r].wait()
        spans = own_spans(r)
        if r == turns - 1:
            edges = sorted({rest, wide, *spans[0]})
            spans = list(zip(edges, edges[1:]))
        for lo, hi in spans:
            value = own_mix[:, lo:hi]
            if hi <= wide:
                value = value + mix_in[0, :, lo:hi].astype(F32)
            if lo >= rest:
                value = value + mix_in[1, :, lo - rest : hi - rest].astype(F32)
            out_ref[:, lo:hi] = value.astype(BF16)

    for k in ORDER:
        for i in range(4):
            post(k, i).wait_send()
        for r in range(turns):
            for copy in returns(k, r):
                copy.wait_send()
            back_own(k, r).wait_send()
            for h in range(2):
                back_side(h, k, r).wait_send()
        for i, view in enumerate((fill_o.at[0], fill_s.at[0, 0], fill_s.at[1, 0])):
            drained(view, yz_s.at[i, k], yz_s.at[i, k], k).wait_send()


def per_device(tokens, norm_gain, expert_ids, route_weight, exp_gate, exp_up, exp_down):
    toks, width = tokens.shape
    half = width // 2
    wide = WIDE * width // 16
    inner = exp_gate.shape[2]
    ids = expert_ids.reshape(TP, toks, TOP).transpose(0, 2, 1)
    weight = route_weight.reshape(TP, toks, TOP).transpose(0, 2, 1)
    vmem, hbm = pl.BlockSpec(memory_space=pltpu.VMEM), pl.BlockSpec(memory_space=pl.ANY)
    dma = pltpu.SemaphoreType.DMA
    group = YC * CAP

    def copies(*lead, size=width):
        return pltpu.VMEM(lead + (YC, PAIRS, 2, size), BF16)

    return pl.pallas_call(
        kernel,
        out_shape=pltpu.VMEM((toks, width), BF16),
        in_specs=[vmem] * 3 + [hbm] * 4,
        out_specs=vmem,
        scratch_shapes=[
            pltpu.VMEM((width, inner), BF16),
            pltpu.VMEM((width, inner), BF16),
            pltpu.VMEM((inner, width), BF16),
            pltpu.VMEM((toks, width), BF16),
            pltpu.VMEM((toks, width), BF16),
            pltpu.VMEM((2, toks, wide), BF16),
            copies(Z),
            copies(2, Z, size=wide),
            copies(TP, Z),
            copies(TP, Z),
            pltpu.VMEM((TP * group, width), BF16),
            pltpu.VMEM((TP * group, inner), BF16),
            copies(Z),
            copies(2, Z, size=half),
            copies(Z),
            copies(2, Z, size=wide),
            pltpu.VMEM((2, Z * group, wide), BF16),
            pltpu.VMEM((2, toks, wide), BF16),
            pltpu.VMEM((2, toks, wide), BF16),
            pltpu.VMEM((3, 2, Z * group, toks), BF16),
            pltpu.VMEM((toks, width), F32),
            dma((4,)),
            dma((2,)),
            dma((2,)),
            dma((3, Z)),
            dma((3, Z)),
            dma((4, Z)),
            dma((4, Z)),
            dma((4, len(CUTS) * Z)),
            dma((4, len(CUTS) * Z)),
            dma((3, len(CUTS) * Z)),
            dma((3, len(CUTS) * Z)),
            dma((2, len(CUTS))),
            dma((2, len(CUTS))),
        ],
        compiler_params=pltpu.CompilerParams(
            collective_id=0, has_side_effects=True, vmem_limit_bytes=63 * 2**20
        ),
    )(ids, weight, norm_gain.reshape(1, width), tokens, exp_gate, exp_up, exp_down)


def solution(mesh):
    return jax.shard_map(
        per_device,
        mesh=mesh,
        in_specs=(
            P(("ep", "tp"), None),
            P(),
            P("ep", None),
            P("ep", None),
            P("ep", None, "tp"),
            P("ep", None, "tp"),
            P("ep", "tp", None),
        ),
        out_specs=P(("ep", "tp"), None),
        check_vma=False,
    )
```
